32 devices in a mesh: sp: 16 (over z, y, x), tp: 2 (over core).
Axes of the slice: x: 2, y: 2, z: 4, core: 2. Of those that a mesh axis runs over, the one named last changes fastest.
Arguments:
- query_logits: bfloat16 [2048, 1024], P('sp', 'tp'), may hold values from -6 to 6
- value_rows: bfloat16 [2048, 1024], P('sp', 'tp'), may hold values from -6 to 6
- onward_forget_logits: bfloat16 [2048, 1024], P('sp', 'tp'), may hold values from -5.5 to 5.5
- reverse_forget_logits: bfloat16 [2048, 1024], P('sp', 'tp'), may hold values from -5.5 to 5.5
- output_gate_logits: bfloat16 [2048, 1024], P('sp', 'tp'), may hold values from -6 to 6
- onward_floor_gap: float32 [1024], P('tp'), may hold values from 0 to 0.12, as said below
- reverse_floor_gap: float32 [1024], P('tp'), may hold values from 0 to 0.12, as said below
- extra_log_decay: float32 [2048, 8], P('sp', 'tp'), may hold values from -2.1 to 0
- per_head_gain: float32 [128], replicated, may hold values from 0.1 to 1.9
- residual: bfloat16 [2048, 2048], P('sp', 'tp'), may hold values from -8 to 8
- output_matrix: bfloat16 [1024, 2048], P(None, 'tp'), may hold values from -0.375 to 0.375
- inner_norm_gain: float32 [2048], P('tp'), may hold values from 0.1 to 1.9
- inner_norm_bias: float32 [2048], P('tp'), may hold values from -1.5 to 1.5
- gate_matrix: bfloat16 [2048, 5632], P('sp', 'tp'), may hold values from -0.125 to 0.125
- up_matrix: bfloat16 [2048, 5632], P('sp', 'tp'), may hold values from -0.125 to 0.125
- down_matrix: bfloat16 [5632, 2048], P('tp', 'sp'), may hold values from -0.15625 to 0.15625
- closing_norm_gain: float32 [2048], P('tp'), may hold values from 0.1 to 1.9
- closing_norm_bias: float32 [2048], P('tp'), may hold values from -1.5 to 1.5
Outputs:
- layer_output: bfloat16 [2048, 2048], P('sp', 'tp')
The draws below stay inside these ranges and needn't reach their ends.
Inputs may be any that keep to these rules, and one draw needn't show every extreme that they name: `onward_floor_gap`: positive. `reverse_floor_gap`: positive.
All inputs are finite; a program needn't handle non-finite values.
Results may differ from the reference program's by a relative error of at most 0.014.
Values may be sent and summed in bfloat16 or wider, within the bound.
A program may use at most 128 MiB of HBM per device.

```python
import math
import jax
import jax.numpy as jnp
from jax import lax

D = 2048
HEADS = 8
HEAD_WIDTH = 128
FF = 5632
TOK_DEV = 128
TOKENS = 2048
N_TP = 2


def forget_values(key):
    block_shift = jax.random.uniform(jax.random.fold_in(key, 11), (TOKENS // TOK_DEV, 1), jnp.float32, -1.5, 1.5)
    shift = jnp.repeat(block_shift, TOK_DEV, axis=0)
    noise = jnp.clip(jax.random.normal(key, (TOKENS, HEADS * HEAD_WIDTH), jnp.float32), -4.0, 4.0)
    return (noise + shift).astype(jnp.bfloat16)


def floor_values(key):
    order = jax.random.permutation(jax.random.fold_in(key, 1), HEADS)
    fast = order < HEADS // 2
    quick = jax.random.uniform(jax.random.fold_in(key, 2), (HEADS, HEAD_WIDTH), jnp.float32, 0.03, 0.12)
    slow = jax.random.uniform(jax.random.fold_in(key, 3), (HEADS, HEAD_WIDTH), jnp.float32, 0.3, 1.2) / TOKENS
    return jnp.where(fast[:, None], quick, slow).reshape(HEADS * HEAD_WIDTH).astype(jnp.float32)


def draw_onward_forget_logits(key, part):
    return forget_values(jax.random.fold_in(key, 101))


def draw_reverse_forget_logits(key, part):
    return forget_values(jax.random.fold_in(key, 202))


def draw_onward_floor_gap(key, part):
    return floor_values(jax.random.fold_in(key, 303))


def draw_reverse_floor_gap(key, part):
    return floor_values(jax.random.fold_in(key, 404))


def draw_extra_log_decay(key, part):
    inner = jax.random.fold_in(key, 505)
    spots = jax.random.randint(jax.random.fold_in(inner, 1), (3, HEADS), 0, TOKENS)
    depth = jnp.log(jax.random.uniform(jax.random.fold_in(inner, 2), (3, HEADS), jnp.float32, 0.5, 0.8))
    places = jnp.arange(TOKENS, dtype=jnp.int32)[:, None, None] == spots[None]
    return jnp.sum(jnp.where(places, depth[None], 0.0), axis=1).astype(jnp.float32)


def draw_residual(key, part):
    inner = jax.random.fold_in(key, 606)
    ramp = 0.6 + 1.2 * jnp.arange(D, dtype=jnp.float32) / D
    base = jax.random.normal(inner, (TOKENS, D), jnp.float32)
    return jnp.clip(base * ramp, -8.0, 8.0).astype(jnp.bfloat16)


def shard_levels(stream_key, extent, pieces, smallest, largest):
    def one(dim, shards_of):
        steps = jax.random.uniform(jax.random.fold_in(jax.random.fold_in(stream_key, 6), dim), (shards_of,), jnp.float32, smallest / len(pieces), largest / len(pieces))
        return jnp.repeat(jnp.exp(steps), extent[dim] // shards_of).reshape((-1,) + (1,) * (len(extent) - dim - 1))

    level = one(*pieces[0])
    for cut in pieces[1:]:
        level = level * one(*cut)
    return level


def bell_draw(key, shape, scale, limit, cuts=(), kind=jnp.bfloat16):
    level = shard_levels(key, shape, cuts, -0.22, 0.18) if cuts else 1.0
    values = jax.random.normal(key, shape, jnp.float32) * scale * level
    return jnp.minimum(jnp.maximum(values, -limit), limit).astype(kind)


def setup_inputs(seed: int = 0) -> dict:
    arg_keys = jax.random.split(jax.random.key(seed), 19)
    return {
        "query_logits": bell_draw(arg_keys[0], (TOKENS, HEADS * HEAD_WIDTH), 1.0, 6.0, ((0, 16), (1, 2))),
        "value_rows": bell_draw(arg_keys[1], (TOKENS, HEADS * HEAD_WIDTH), 1.0, 6.0, ((0, 16), (1, 2))),
        "onward_forget_logits": draw_onward_forget_logits(jax.random.fold_in(arg_keys[18], 71), 0),
        "reverse_forget_logits": draw_reverse_forget_logits(jax.random.fold_in(arg_keys[18], 71), 0),
        "output_gate_logits": bell_draw(arg_keys[4], (TOKENS, HEADS * HEAD_WIDTH), 1.0, 6.0, ((0, 16), (1, 2))),
        "onward_floor_gap": draw_onward_floor_gap(jax.random.fold_in(arg_keys[18], 71), 0),
        "reverse_floor_gap": draw_reverse_floor_gap(jax.random.fold_in(arg_keys[18], 71), 0),
        "extra_log_decay": draw_extra_log_decay(jax.random.fold_in(arg_keys[18], 71), 0),
        "per_head_gain": jnp.clip(1.0 + 0.18 * jax.random.normal(arg_keys[8], (HEAD_WIDTH,), jnp.float32), 0.1, 1.9),
        "residual": draw_residual(jax.random.fold_in(arg_keys[18], 71), 0),
        "output_matrix": bell_draw(arg_keys[10], (HEADS * HEAD_WIDTH, D), (HEADS * HEAD_WIDTH // 4) ** -0.5, 0.375, ((1, 2),)),
        "inner_norm_gain": jnp.clip(1.0 + 0.18 * jax.random.normal(arg_keys[11], (D,), jnp.float32), 0.1, 1.9),
        "inner_norm_bias": bell_draw(arg_keys[12], (D,), 0.3, 1.5, ((0, 2),), jnp.float32),
        "gate_matrix": bell_draw(arg_keys[13], (D, FF), D ** -0.5, 0.125, ((0, 16), (1, 2))),
        "up_matrix": bell_draw(arg_keys[14], (D, FF), D ** -0.5, 0.125, ((0, 16), (1, 2))),
        "down_matrix": bell_draw(arg_keys[15], (FF, D), (FF // 4) ** -0.5, 0.15625, ((0, 2), (1, 16))),
        "closing_norm_gain": jnp.clip(1.0 + 0.18 * jax.random.normal(arg_keys[16], (D,), jnp.float32), 0.1, 1.9),
        "closing_norm_bias": bell_draw(arg_keys[17], (D,), 0.3, 1.5, ((0, 2),), jnp.float32),
    }


highest_precision = lax.Precision.HIGHEST
alpha_mix = 2.0 ** 0.25
norm_eps = 1e-05
head_eps = 1e-06

def decay_factors(unscaled_input, lower_bound_gap, extra_decays):
    decay_factor = lower_bound_gap * jax.nn.sigmoid(-unscaled_input.astype(jnp.float32))
    return (jnp.log1p(-decay_factor) + extra_decays, decay_factor)

def recurrence(query, keys, values, log_decay):
    total, head_count, model_width = query.shape
    span = math.gcd(total, 128)
    count = total // span
    triangle = jnp.tril(jnp.ones((span, span), jnp.float32))

    def blocks(array):
        return array.reshape(count, span, head_count, array.shape[2])

    def advance(running_state, inputs):
        query_block, key_block, value_tile, log_block = inputs
        running = jnp.cumsum(log_block, axis=0)
        final_index = running[-1]
        decayed_query = query_block * jnp.exp(running)
        key_inverse = key_block * jnp.exp(-running)
        key_stop = key_block * jnp.exp(final_index[None] - running)
        scores = jnp.einsum('thk,shk->hts', decayed_query, key_inverse, precision=highest_precision) * triangle[None]
        inner = jnp.einsum('hts,shv->thv', scores, value_tile, precision=highest_precision)
        carried_state = jnp.einsum('nex,exl->nel', decayed_query, running_state, precision=highest_precision)
        running_state = jnp.exp(final_index)[:, :, None] * running_state + jnp.einsum('ojy,oje->jye', key_stop, value_tile, precision=highest_precision)
        return (running_state, inner + carried_state)
    start = jnp.zeros((head_count, model_width, values.shape[2]), jnp.float32)
    final, outputs = lax.scan(advance, start, (blocks(query), blocks(keys), blocks(values), blocks(log_decay)))
    return outputs.reshape(total, head_count, values.shape[2])

def layer_norm(rows, gain, bias):
    centre = rows - lax.optimization_barrier(jnp.mean(rows, axis=-1, keepdims=True))
    spread = lax.optimization_barrier(jnp.mean(centre * centre, axis=-1, keepdims=True))
    return centre * lax.rsqrt(spread + norm_eps) * gain + bias

def reference(query_logits, value_rows, onward_forget_logits, reverse_forget_logits, output_gate_logits, onward_floor_gap, reverse_floor_gap, extra_log_decay, per_head_gain, residual, output_matrix, inner_norm_gain, inner_norm_bias, gate_matrix, up_matrix, down_matrix, closing_norm_gain, closing_norm_bias):
    total = query_logits.shape[0]
    shape_head = (total, HEADS, HEAD_WIDTH)
    query = jax.nn.silu(query_logits.astype(jnp.float32)).reshape(shape_head)
    values = value_rows.astype(jnp.float32).reshape(shape_head)
    extra_decays = jnp.repeat(extra_log_decay, HEAD_WIDTH, axis=1)
    onward_log_decay, onward_key_rows = decay_factors(onward_forget_logits, onward_floor_gap, extra_decays)
    reverse_log_decay, reverse_key_rows = decay_factors(reverse_forget_logits, reverse_floor_gap, extra_decays)
    upcoming_part = recurrence(query, onward_key_rows.reshape(shape_head), values, onward_log_decay.reshape(shape_head))
    preceding_part = jnp.flip(recurrence(jnp.flip(query, axis=0), jnp.flip(reverse_key_rows.reshape(shape_head), axis=0), jnp.flip(values, axis=0), jnp.flip(reverse_log_decay.reshape(shape_head), axis=0)), axis=0)
    mixed = upcoming_part + preceding_part
    normed = mixed * lax.rsqrt(lax.optimization_barrier(jnp.mean(mixed * mixed, axis=2, keepdims=True)) + head_eps) * per_head_gain
    gated = (normed.reshape(total, HEADS * HEAD_WIDTH) * jax.nn.silu(output_gate_logits.astype(jnp.float32))).astype(jnp.bfloat16)
    piece_rows = math.gcd(total, 2048)
    count = total // piece_rows
    share = FF // N_TP

    def finish(inputs):
        gated_rows, residual_rows = inputs
        mixer = jnp.dot(gated_rows, output_matrix, preferred_element_type=jnp.float32)
        middle = layer_norm(alpha_mix * residual_rows.astype(jnp.float32) + mixer, inner_norm_gain, inner_norm_bias).astype(jnp.bfloat16)
        gate = jnp.dot(middle, gate_matrix, preferred_element_type=jnp.float32)
        up = jnp.dot(middle, up_matrix, preferred_element_type=jnp.float32)
        hidden = (jax.nn.silu(gate) * up).astype(jnp.bfloat16)
        feed = jnp.zeros((piece_rows, D), jnp.float32)
        for part_index in range(N_TP):
            term = jnp.dot(hidden[:, part_index * share:(part_index + 1) * share], down_matrix[part_index * share:(part_index + 1) * share], preferred_element_type=jnp.float32).astype(jnp.bfloat16)
            feed = feed + lax.optimization_barrier(term).astype(jnp.float32)
        return layer_norm(alpha_mix * middle.astype(jnp.float32) + feed, closing_norm_gain, closing_norm_bias).astype(jnp.bfloat16)
    result = lax.map(finish, (gated.reshape(count, piece_rows, HEADS * HEAD_WIDTH), residual.reshape(count, piece_rows, D)))
    return result.reshape(total, D)
```

```python
import functools
import math

import jax
import jax.numpy as jnp
from jax import lax
from jax.experimental import pallas as pl
from jax.experimental.pallas import tpu as pltpu
from jax.sharding import PartitionSpec as P


highest = lax.Precision.HIGHEST
alpha_mix = 2.0**0.25
norm_eps = 1e-05
head_eps = 1e-06
bf16 = jnp.bfloat16
f32 = jnp.float32


def bits_of(count):
    return [1 << k for k in range(count.bit_length() - 1)]


def swap(x, axis, mask):
    count = lax.axis_size(axis)
    return lax.ppermute(x, axis, [(i, i ^ mask) for i in range(count)])


def unxor(blocks, place):
    for bit in bits_of(len(blocks)):
        odd = (place & bit) != 0
        blocks = [jnp.where(odd, blocks[p ^ bit], blocks[p]) for p in range(len(blocks))]
    return blocks


def tp_blocks(x):
    return [x] + [swap(x, "tp", m) for m in range(1, lax.axis_size("tp"))]


def tp_whole(x, axis):
    return jnp.concatenate(unxor(tp_blocks(x), lax.axis_index("tp")), axis=axis)


def local_kernel(heads, q_ref, v_ref, f_ref, r_ref, fg_ref, rg_ref, ex_ref,
                 inner_ref, df_ref, db_ref, state_ref, total_ref):
    rows = q_ref.shape[0]
    width = q_ref.shape[1] // heads
    t = lax.broadcasted_iota(jnp.int32, (rows, rows), 0)
    s = lax.broadcasted_iota(jnp.int32, (rows, rows), 1)
    lower, upper = s <= t, s >= t
    for h in range(heads):
        cols = pl.ds(h * width, width)
        ql = q_ref[:, cols].astype(f32)
        q = ql / (1.0 + jnp.exp(-ql))
        v = v_ref[:, cols]
        extra = ex_ref[:, pl.ds(h, 1)]
        scores = jnp.zeros((rows, rows), f32)
        for d, (raw_ref, gap_ref, tri, d_ref) in enumerate(
            ((f_ref, fg_ref, lower, df_ref), (r_ref, rg_ref, upper, db_ref))
        ):
            raw = raw_ref[:, cols].astype(f32)
            key = gap_ref[:, cols] * (1.0 / (1.0 + jnp.exp(raw)))
            log = jnp.log1p(-key) + extra
            run = jnp.dot(tri.astype(f32), log, precision=highest, preferred_element_type=f32)
            last = run[rows - 1 :, :] if d == 0 else run[:1, :]
            dq = (q * jnp.exp(run)).astype(bf16)
            ki = (key * jnp.exp(-run)).astype(bf16)
            ks = (key * jnp.exp(last - run)).astype(bf16)
            part = lax.dot_general(dq, ki, (((1,), (1,)), ((), ())), preferred_element_type=f32)
            scores = scores + jnp.where(tri, part, 0.0)
            d_ref[:, cols] = dq
            state_ref[d, h] = lax.dot_general(
                ks, v, (((0,), (0,)), ((), ())), preferred_element_type=f32
            )
            total_ref[d, pl.ds(h, 1), :] = last
        inner_ref[:, cols] = jnp.dot(scores.astype(bf16), v, preferred_element_type=f32)


def mix_kernel(heads, inner_ref, df_ref, db_ref, state_ref, gate_ref, gain_ref, out_ref):
    width = inner_ref.shape[1] // heads
    for h in range(heads):
        cols = pl.ds(h * width, width)
        mixed = (
            inner_ref[:, cols]
            + jnp.dot(df_ref[:, cols], state_ref[0, h].astype(bf16), preferred_element_type=f32)
            + jnp.dot(db_ref[:, cols], state_ref[1, h].astype(bf16), preferred_element_type=f32)
        )
        normed = (
            mixed
            * lax.rsqrt(jnp.mean(mixed * mixed, axis=1, keepdims=True) + head_eps)
            * gain_ref[...]
        )
        gl = gate_ref[:, cols].astype(f32)
        out_ref[:, cols] = (normed * (gl / (1.0 + jnp.exp(-gl)))).astype(bf16)


def call(body, outs, *args):
    flops = sum(2 * math.prod(o.shape) * 128 for o in outs)
    size = sum(math.prod(a.shape) * a.dtype.itemsize for a in list(outs) + list(args))
    return pl.pallas_call(
        body,
        out_shape=tuple(outs),
        cost_estimate=pl.CostEstimate(flops=flops, bytes_accessed=size * 4, transcendentals=0),
    )(*args)


def prefix(state, total):
    count = lax.axis_size("sp")
    me = lax.axis_index("sp")
    before, before_total = jnp.zeros_like(state), jnp.zeros_like(total)
    steps = bits_of(count)
    for bit in steps:
        high = (me & bit) != 0
        takes = jnp.stack([high, jnp.logical_not(high)])
        if bit == steps[-1]:
            sent = jnp.where(high, state[1], state[0]).astype(bf16)
            came = swap(sent, "sp", bit).astype(f32)[None]
            joined = jnp.exp(before_total)[..., None] * came + before
            return jnp.where(takes[:, None, None, None], joined, before)
        came = swap(state.astype(bf16), "sp", bit).astype(f32)
        came_total = swap(total, "sp", bit)
        t3, t4 = takes[:, None, None], takes[:, None, None, None]
        before = jnp.where(t4, jnp.exp(before_total)[..., None] * came + before, before)
        before_total = jnp.where(t3, before_total + came_total, before_total)
        state = jnp.where(
            t4,
            jnp.exp(total)[..., None] * came + state,
            jnp.exp(came_total)[..., None] * state + came,
        )
        total = total + came_total
    return before


def spread(pieces, near, order):
    blocks = {0: pieces}
    for bit in order:
        blocks.update({m ^ bit: swap(b, "sp", bit) for m, b in list(blocks.items())})
    return [blocks[j] for j in range(near)]


def layer_norm(x, gain, bias):
    mean = jnp.mean(x, axis=1, keepdims=True)
    centre = x - mean
    var = jnp.mean(centre * centre, axis=1, keepdims=True)
    return centre * lax.rsqrt(var + norm_eps) * gain + bias


def shards(
    query_logits, value_rows, onward_forget_logits, reverse_forget_logits, output_gate_logits,
    onward_floor_gap, reverse_floor_gap, extra_log_decay, per_head_gain, residual, output_matrix,
    inner_norm_gain, inner_norm_bias, gate_matrix, up_matrix, down_matrix,
    closing_norm_gain, closing_norm_bias,
):
    count, cores = lax.axis_size("sp"), lax.axis_size("tp")
    me, core = lax.axis_index("sp"), lax.axis_index("tp")
    far = math.gcd(count, 4)
    near = count // far
    rows, width = query_logits.shape
    heads = extra_log_decay.shape[1]
    chan = width // heads
    model = residual.shape[1] * cores
    slab = model // count
    units = gate_matrix.shape[1] // far
    place = me // near

    inner, df, db, state, total = call(
        functools.partial(local_kernel, heads),
        (
            jax.ShapeDtypeStruct((rows, width), f32),
            jax.ShapeDtypeStruct((rows, width), bf16),
            jax.ShapeDtypeStruct((rows, width), bf16),
            jax.ShapeDtypeStruct((2, heads, chan, chan), f32),
            jax.ShapeDtypeStruct((2, heads, chan), f32),
        ),
        query_logits, value_rows, onward_forget_logits, reverse_forget_logits,
        onward_floor_gap[None], reverse_floor_gap[None], extra_log_decay,
    )

    def dealt(matrix, axis):
        pieces = []
        for s in range(far):
            piece = lax.dynamic_slice_in_dim(matrix, (place ^ s) * units, units, axis)
            pieces.append(swap(piece, "sp", s * near) if s else piece)
        return jnp.stack(pieces)

    bits = bits_of(near)
    gates = spread(dealt(gate_matrix, 1), near, bits)
    ups = spread(dealt(up_matrix, 1), near, bits[::-1])
    downs = dealt(down_matrix, 0)
    half = units // 2
    downs = [
        jnp.concatenate(pair, axis=1)
        for pair in zip(
            spread(downs[:, :half], near, bits), spread(downs[:, half:], near, bits[::-1])
        )
    ]
    slots = [(s, j) for s in range(far) for j in range(near)]
    gate_whole = jnp.concatenate([gates[j][s] for s, j in slots], axis=0)
    up_whole = jnp.concatenate([ups[j][s] for s, j in slots], axis=0)
    down_whole = jnp.concatenate([downs[j][s] for s, j in slots], axis=1)

    residual_whole = tp_whole(residual, 1).astype(f32)
    inner_gain, inner_bias, closing_gain, closing_bias = jnp.split(
        tp_whole(
            jnp.stack([inner_norm_gain, inner_norm_bias, closing_norm_gain, closing_norm_bias]), 1
        ),
        4,
    )
    output_blocks = tp_blocks(output_matrix)

    before = prefix(state, total)
    (gated,) = call(
        functools.partial(mix_kernel, heads),
        (jax.ShapeDtypeStruct((rows, width), bf16),),
        inner, df, db, before, output_gate_logits, per_head_gain[None],
    )
    gated = tp_whole(gated, 1)
    mixer = jnp.concatenate(
        unxor([jnp.dot(gated, b, preferred_element_type=f32) for b in output_blocks], core), axis=1
    )
    middle = layer_norm(alpha_mix * residual_whole + mixer, inner_gain, inner_bias).astype(bf16)

    def part(x, m):
        return x[:, m * slab : (m + 1) * slab]

    def turned(x, s):
        return jnp.concatenate([part(x, m ^ (s * near)) for m in range(count)], axis=1)

    ordered = jnp.concatenate(
        [lax.dynamic_slice_in_dim(middle, (me ^ m) * slab, slab, 1) for m in range(count)], axis=1
    )
    share = model // cores
    arrived = []
    for s in range(far):
        piece = lax.dynamic_slice_in_dim(turned(ordered, s), core * share, share, 1)
        arrived.append(swap(piece, "sp", s * near) if s else piece)
    whole = tp_whole(jnp.concatenate(arrived, axis=0), 1)

    gate = jnp.dot(whole, gate_whole, preferred_element_type=f32)
    up = jnp.dot(whole, up_whole, preferred_element_type=f32)
    hidden = (gate / (1.0 + jnp.exp(-gate)) * up).astype(bf16)
    partial_value = jnp.dot(hidden, down_whole, preferred_element_type=f32).astype(bf16)

    partial_value = jnp.concatenate(
        [turned(partial_value[s * rows : (s + 1) * rows], s) for s in range(far)], axis=0
    )
    feed = lax.dynamic_slice_in_dim(partial_value, core * share, share, 1).astype(f32)
    for m in range(1, cores):
        feed = feed + swap(
            lax.dynamic_slice_in_dim(partial_value, (core ^ m) * share, share, 1), "tp", m
        ).astype(f32)
    feed = feed.astype(bf16)
    mine = feed[:rows].astype(f32)
    for s in range(1, far):
        mine = mine + swap(feed[s * rows : (s + 1) * rows], "sp", s * near).astype(f32)
    mine = tp_whole(mine.astype(bf16), 1)
    total_feed = jnp.concatenate(
        [lax.dynamic_slice_in_dim(mine, (me ^ p) * slab, slab, 1) for p in range(count)], axis=1
    ).astype(f32)
    final = layer_norm(alpha_mix * middle.astype(f32) + total_feed, closing_gain, closing_bias)
    return lax.dynamic_slice_in_dim(final, core * share, share, 1).astype(bf16)


def solution(mesh):
    a, b = P("sp", "tp"), P("tp")
    placed = (a, a, a, a, a, b, b, a, P(), a, P(None, "tp"), b, b, a, a, P("tp", "sp"), b, b)
    return jax.shard_map(
        shards, mesh=mesh, in_specs=placed, out_specs=P("sp", "tp"), check_vma=False
    )
```

```python
import functools
import math

import jax
import jax.numpy as jnp
from jax import lax
from jax.experimental import pallas as pl
from jax.experimental.pallas import tpu as pltpu
from jax.sharding import PartitionSpec as P


highest = lax.Precision.HIGHEST
alpha_mix = 2.0**0.25
norm_eps = 1e-05
head_eps = 1e-06
bf16 = jnp.bfloat16
f32 = jnp.float32


def bits_of(count):
    return [1 << k for k in range(count.bit_length() - 1)]


def swap(x, axis, mask):
    count = lax.axis_size(axis)
    return lax.ppermute(x, axis, [(i, i ^ mask) for i in range(count)])


def unxor(blocks, place):
    for bit in bits_of(len(blocks)):
        odd = (place & bit) != 0
        blocks = [jnp.where(odd, blocks[p ^ bit], blocks[p]) for p in range(len(blocks))]
    return blocks


def tp_blocks(x):
    return [x] + [swap(x, "tp", m) for m in range(1, lax.axis_size("tp"))]


def tp_whole(x, axis):
    return jnp.concatenate(unxor(tp_blocks(x), lax.axis_index("tp")), axis=axis)


def pack(send_ref, d, h, state, last):
    width = state.shape[0]
    send_ref[d, h, pl.ds(0, width), :] = state.astype(bf16)
    head = last.astype(bf16)
    rest = last - head.astype(f32)
    row = lax.broadcasted_iota(jnp.int32, (16, width), 0)
    tail = jnp.where(row == 0, head.astype(f32), jnp.where(row == 1, rest, 0.0))
    send_ref[d, h, pl.ds(width, 16), :] = tail.astype(bf16)


def join_kernel(bit, after, first, came_ref, state_ref, total_ref, before_ref, btotal_ref,
                nstate_ref, ntotal_ref, nbefore_ref, nbtotal_ref, send_ref):
    heads, width = total_ref.shape[1:]
    me = lax.axis_index("sp")
    high = (me & bit) != 0
    for h in range(heads):
        states = []
        for d in range(2):
            takes = high if d == 0 else jnp.logical_not(high)
            came = came_ref[d, h, pl.ds(0, width), :].astype(f32)
            tail = came_ref[d, h, pl.ds(width, 16), :].astype(f32)
            came_total = tail[:1] + tail[1:2]
            state, total = state_ref[d, h], total_ref[d, pl.ds(h, 1), :]
            if first:
                before, btotal = jnp.zeros_like(state), jnp.zeros_like(total)
            else:
                before, btotal = before_ref[d, h], btotal_ref[d, pl.ds(h, 1), :]
            nbefore_ref[d, h] = jnp.where(takes, jnp.exp(btotal) * came + before, before)
            nbtotal_ref[d, pl.ds(h, 1), :] = jnp.where(takes, btotal + came_total, btotal)
            state = jnp.where(
                takes, jnp.exp(total) * came + state, jnp.exp(came_total) * state + came
            )
            total = total + came_total
            nstate_ref[d, h] = state
            ntotal_ref[d, pl.ds(h, 1), :] = total
            states.append(state)
            if after is None:
                pack(send_ref, d, h, state, total)
        if after is not None:
            send_ref[h] = jnp.where((me & after) != 0, states[1], states[0]).astype(bf16)


def local_kernel(heads, q_ref, v_ref, f_ref, r_ref, fg_ref, rg_ref, ex_ref,
                 inner_ref, df_ref, db_ref, state_ref, total_ref, send_ref):
    rows = q_ref.shape[0]
    width = q_ref.shape[1] // heads
    t = lax.broadcasted_iota(jnp.int32, (rows, rows), 0)
    s = lax.broadcasted_iota(jnp.int32, (rows, rows), 1)
    lower, upper = s <= t, s >= t
    for h in range(heads):
        cols = pl.ds(h * width, width)
        ql = q_ref[:, cols].astype(f32)
        q = ql / (1.0 + jnp.exp(-ql))
        v = v_ref[:, cols]
        extra = ex_ref[:, pl.ds(h, 1)]
        scores = jnp.zeros((rows, rows), f32)
        for d, (raw_ref, gap_ref, tri, d_ref) in enumerate(
            ((f_ref, fg_ref, lower, df_ref), (r_ref, rg_ref, upper, db_ref))
        ):
            raw = raw_ref[:, cols].astype(f32)
            key = gap_ref[:, cols] * (1.0 / (1.0 + jnp.exp(raw)))
            log = jnp.log1p(-key) + extra
            run = jnp.dot(tri.astype(f32), log, precision=highest, preferred_element_type=f32)
            last = run[rows - 1 :, :] if d == 0 else run[:1, :]
            dq = (q * jnp.exp(run)).astype(bf16)
            ki = (key * jnp.exp(-run)).astype(bf16)
            ks = (key * jnp.exp(last - run)).astype(bf16)
            part = lax.dot_general(dq, ki, (((1,), (1,)), ((), ())), preferred_element_type=f32)
            scores = scores + jnp.where(tri, part, 0.0)
            d_ref[:, cols] = dq
            state = lax.dot_general(v, ks, (((0,), (0,)), ((), ())), preferred_element_type=f32)
            state_ref[d, h] = state
            total_ref[d, pl.ds(h, 1), :] = last
            pack(send_ref, d, h, state, last)
        inner_ref[:, cols] = jnp.dot(scores.astype(bf16), v, preferred_element_type=f32)


def mix_kernel(bit, heads, inner_ref, df_ref, db_ref, came_ref, before_ref, btotal_ref,
               gate_ref, gain_ref, out_ref):
    width = inner_ref.shape[1] // heads
    high = (lax.axis_index("sp") & bit) != 0
    for h in range(heads):
        cols = pl.ds(h * width, width)
        mixed = inner_ref[:, cols]
        came = came_ref[h].astype(f32)
        for d, d_ref in enumerate((df_ref, db_ref)):
            takes = high if d == 0 else jnp.logical_not(high)
            before = before_ref[d, h]
            state = jnp.where(
                takes, jnp.exp(btotal_ref[d, pl.ds(h, 1), :]) * came + before, before
            )
            mixed = mixed + lax.dot_general(
                d_ref[:, cols], state.astype(bf16), (((1,), (1,)), ((), ())),
                preferred_element_type=f32,
            )
        normed = (
            mixed
            * lax.rsqrt(jnp.mean(mixed * mixed, axis=1, keepdims=True) + head_eps)
            * gain_ref[...]
        )
        gl = gate_ref[:, cols].astype(f32)
        out_ref[:, cols] = (normed * (gl / (1.0 + jnp.exp(-gl)))).astype(bf16)


def ordered(x, far, near, place):
    rows, model = x.shape
    slab = model // (far * near)
    blocks = [
        jnp.concatenate(
            [x[:, (z * near + r) * slab : (z * near + r + 1) * slab] for z in range(far)], axis=1
        )
        for r in range(near)
    ]
    return unxor(blocks, place)


def unordered(blocks, far, near, place):
    blocks = unxor(blocks, place)
    slab = blocks[0].shape[1] // far
    return jnp.concatenate(
        [blocks[r][:, z * slab : (z + 1) * slab] for z in range(far) for r in range(near)], axis=1
    )


def middle_kernel(cores, far, near, *refs):
    gated, output, residual, gains, biases = (refs[i * cores : (i + 1) * cores] for i in range(5))
    middle_ref, send_ref = refs[5 * cores :]
    core = lax.axis_index("tp")
    width = gated[0].shape[1]
    parts = []
    for b in range(cores):
        mixer = alpha_mix * residual[b][...].astype(f32)
        for m in range(cores):
            at = pl.ds(pl.multiple_of((core ^ m) * width, width), width)
            mixer = mixer + jnp.dot(gated[m][...], output[b][at, :], preferred_element_type=f32)
        parts.append(mixer)
    model = cores * parts[0].shape[1]
    mean = sum(jnp.sum(p, axis=1, keepdims=True) for p in parts) / model
    parts = [p - mean for p in parts]
    var = sum(jnp.sum(p * p, axis=1, keepdims=True) for p in parts) / model
    scale = lax.rsqrt(var + norm_eps)
    parts = [p * scale * gains[b][...] + biases[b][...] for b, p in enumerate(parts)]
    whole = jnp.concatenate(unxor(parts, core), axis=1)
    middle_ref[...] = whole.astype(bf16)
    near_place = lax.rem(lax.axis_index("sp"), near)
    blocks = ordered(whole.astype(bf16).astype(f32), far, near, near_place)
    share = near // cores
    halves = [
        jnp.concatenate(blocks[c * share : (c + 1) * share], axis=1) for c in range(cores)
    ]
    send_ref[...] = unxor(halves, core)[0].astype(bf16)


def forward_kernel(cores, near, *refs):
    rows = refs[:cores]
    gates, ups, first, second = (
        refs[cores + i * near : cores + (i + 1) * near] for i in range(4)
    )
    outs = refs[cores + 4 * near :]
    core = lax.axis_index("tp")
    share = near // cores
    deep = gates[0].shape[0]
    lanes = unxor([r[...] for r in rows], core)
    gate = up = 0.0
    for j in range(near):
        x = lanes[j // share][:, (j % share) * deep : (j % share + 1) * deep]
        gate = gate + jnp.dot(x, gates[j][...], preferred_element_type=f32)
        up = up + jnp.dot(x, ups[j][...], preferred_element_type=f32)
    hidden = (gate / (1.0 + jnp.exp(-gate)) * up).astype(bf16)
    half = first[0].shape[0]
    a, b = hidden[:, :half], hidden[:, half:]
    halves = []
    for c in range(cores):
        halves.append(
            jnp.concatenate(
                [
                    jnp.dot(a, first[j][...], preferred_element_type=f32)
                    + jnp.dot(b, second[j][...], preferred_element_type=f32)
                    for j in range(c * share, (c + 1) * share)
                ],
                axis=1,
            ).astype(bf16)
        )
    for out, y in zip(outs, unxor(halves, core)):
        out[...] = y


def final_kernel(cores, far, near, *refs):
    feeds = refs[:cores]
    middle_ref, gain_ref, bias_ref, out_ref = refs[cores:]
    core = lax.axis_index("tp")
    near_place = lax.rem(lax.axis_index("sp"), near)
    whole = unxor([f[...].astype(f32) for f in feeds], core)
    share = near // cores
    deep = whole[0].shape[1] // share
    blocks = [
        whole[j // share][:, (j % share) * deep : (j % share + 1) * deep] for j in range(near)
    ]
    x = alpha_mix * middle_ref[...].astype(f32) + unordered(blocks, far, near, near_place)
    mean = jnp.mean(x, axis=1, keepdims=True)
    x = x - mean
    x = x * lax.rsqrt(jnp.mean(x * x, axis=1, keepdims=True) + norm_eps)
    width = out_ref.shape[1]
    mine = unxor([x[:, c * width : (c + 1) * width] for c in range(cores)], core)[0]
    out_ref[...] = (mine * gain_ref[...] + bias_ref[...]).astype(bf16)


def call(body, outs, *args, flops=0):
    size = sum(math.prod(a.shape) * a.dtype.itemsize for a in list(outs) + list(args))
    return pl.pallas_call(
        body,
        out_shape=tuple(outs),
        cost_estimate=pl.CostEstimate(flops=flops, bytes_accessed=size * 4, transcendentals=0),
        compiler_params=pltpu.CompilerParams(vmem_limit_bytes=56 * 1024 * 1024),
    )(*args)


def spread(pieces, near, order):
    blocks = {0: pieces}
    for bit in order:
        blocks.update({m ^ bit: swap(b, "sp", bit) for m, b in list(blocks.items())})
    return [blocks[j] for j in range(near)]


def shards(
    query_logits, value_rows, onward_forget_logits, reverse_forget_logits, output_gate_logits,
    onward_floor_gap, reverse_floor_gap, extra_log_decay, per_head_gain, residual, output_matrix,
    inner_norm_gain, inner_norm_bias, gate_matrix, up_matrix, down_matrix,
    closing_norm_gain, closing_norm_bias,
):
    count, cores = lax.axis_size("sp"), lax.axis_size("tp")
    me, core = lax.axis_index("sp"), lax.axis_index("tp")
    far = math.gcd(count, 4)
    near = count // far
    rows, width = query_logits.shape
    heads = extra_log_decay.shape[1]
    chan = width // heads
    share = residual.shape[1]
    model = share * cores
    units = gate_matrix.shape[1] // far
    place = me // near
    like = jax.ShapeDtypeStruct
    states = (like((2, heads, chan, chan), f32), like((2, heads, chan), f32))
    packed = like((2, heads, chan + 16, chan), bf16)

    inner, df, db, state, total, sent = call(
        functools.partial(local_kernel, heads),
        (like((rows, width), f32), like((rows, width), bf16), like((rows, width), bf16))
        + states + (packed,),
        query_logits, value_rows, onward_forget_logits, reverse_forget_logits,
        onward_floor_gap[None], reverse_floor_gap[None], extra_log_decay,
    )

    def dealt(cut):
        blocks = [swap(cut(place ^ s), "sp", s * near) if s else cut(place) for s in range(far)]
        return unxor(blocks, place)

    both = dealt(
        lambda z: jnp.stack(
            [lax.dynamic_slice_in_dim(w, z * units, units, 1) for w in (gate_matrix, up_matrix)]
        )
    )
    down = dealt(lambda z: lax.dynamic_slice_in_dim(down_matrix, z * units, units, 0))
    half = (units // 2 + 127) // 128 * 128
    bits = bits_of(near)
    gates = spread(jnp.concatenate([b[0] for b in both], axis=0), near, bits)
    ups = spread(jnp.concatenate([b[1] for b in both], axis=0), near, bits[::-1])
    first = spread(jnp.concatenate([d[:half] for d in down], axis=1), near, bits)
    second = spread(jnp.concatenate([d[half:] for d in down], axis=1), near, bits[::-1])

    residuals = tp_blocks(residual)
    vectors = tp_blocks(jnp.stack([inner_norm_gain, inner_norm_bias]))
    outputs = tp_blocks(output_matrix)

    steps = bits_of(count)
    before, before_total = state, total
    for i, bit in enumerate(steps[:-1]):
        last = i == len(steps) - 2
        state, total, before, before_total, sent = call(
            functools.partial(join_kernel, bit, steps[-1] if last else None, i == 0),
            states + states + (like((heads, chan, chan), bf16) if last else packed,),
            swap(sent, "sp", bit), state, total, before, before_total,
        )
    (gated,) = call(
        functools.partial(mix_kernel, steps[-1], heads),
        (like((rows, width), bf16),),
        inner, df, db, swap(sent, "sp", steps[-1]), before, before_total,
        output_gate_logits, per_head_gain[None],
    )
    middle, ready = call(
        functools.partial(middle_kernel, cores, far, near),
        (like((rows, model), bf16), like((rows, share), bf16)),
        *tp_blocks(gated), *outputs, *residuals, *[v[:1] for v in vectors],
        *[v[1:] for v in vectors],
        flops=2 * rows * width * cores * model,
    )

    lines = jnp.concatenate(
        [ready] + [swap(ready, "sp", s * near) for s in range(1, far)], axis=0
    )
    sums = call(
        functools.partial(forward_kernel, cores, near),
        [like((far * rows, share), bf16)] * cores,
        *tp_blocks(lines), *gates, *ups, *first, *second,
        flops=6 * far * rows * model * units,
    )
    feed = sums[0].astype(f32)
    for m in range(1, cores):
        feed = feed + swap(sums[m], "tp", m).astype(f32)
    feed = feed.astype(bf16)
    mine = feed[:rows].astype(f32)
    for s in range(1, far):
        mine = mine + swap(feed[s * rows : (s + 1) * rows], "sp", s * near).astype(f32)
    (out,) = call(
        functools.partial(final_kernel, cores, far, near),
        (like((rows, share), bf16),),
        *tp_blocks(mine.astype(bf16)), middle, closing_norm_gain[None], closing_norm_bias[None],
    )
    return out


def solution(mesh):
    a, b = P("sp", "tp"), P("tp")
    placed = (a, a, a, a, a, b, b, a, P(), a, P(None, "tp"), b, b, a, a, P("tp", "sp"), b, b)
    return jax.shard_map(
        shards, mesh=mesh, in_specs=placed, out_specs=P("sp", "tp"), check_vma=False
    )
```

```python
import functools
import math

import jax
import jax.numpy as jnp
from jax import lax
from jax.experimental import pallas as pl
from jax.experimental.pallas import tpu as pltpu
from jax.sharding import PartitionSpec as P


highest = lax.Precision.HIGHEST
alpha_mix = 2.0**0.25
norm_eps = 1e-05
head_eps = 1e-06
bf16 = jnp.bfloat16
f32 = jnp.float32


def bits_of(count):
    return [1 << k for k in range(count.bit_length() - 1)]


def swap(x, axis, mask):
    count = lax.axis_size(axis)
    return lax.ppermute(x, axis, [(i, i ^ mask) for i in range(count)])


def unxor(blocks, place):
    for bit in bits_of(len(blocks)):
        odd = (place & bit) != 0
        blocks = [jnp.where(odd, blocks[p ^ bit], blocks[p]) for p in range(len(blocks))]
    return blocks


def tp_blocks(x):
    return [x] + [swap(x, "tp", m) for m in range(1, lax.axis_size("tp"))]


def pack(send_ref, d, h, state, last):
    width = state.shape[0]
    send_ref[d, h, pl.ds(0, width), :] = state.astype(bf16)
    head = last.astype(bf16)
    rest = last - head.astype(f32)
    row = lax.broadcasted_iota(jnp.int32, (16, width), 0)
    tail = jnp.where(row == 0, head.astype(f32), jnp.where(row == 1, rest, 0.0))
    send_ref[d, h, pl.ds(width, 16), :] = tail.astype(bf16)


def join_kernel(bit, after, first, came_ref, state_ref, total_ref, before_ref, btotal_ref,
                nstate_ref, ntotal_ref, nbefore_ref, nbtotal_ref, send_ref):
    heads, width = total_ref.shape[1:]
    me = lax.axis_index("sp")
    high = (me & bit) != 0
    for h in range(heads):
        states = []
        for d in range(2):
            takes = high if d == 0 else jnp.logical_not(high)
            came = came_ref[d, h, pl.ds(0, width), :].astype(f32)
            tail = came_ref[d, h, pl.ds(width, 16), :].astype(f32)
            came_total = tail[:1] + tail[1:2]
            state, total = state_ref[d, h], total_ref[d, pl.ds(h, 1), :]
            if first:
                before, btotal = jnp.zeros_like(state), jnp.zeros_like(total)
            else:
                before, btotal = before_ref[d, h], btotal_ref[d, pl.ds(h, 1), :]
            nbefore_ref[d, h] = jnp.where(takes, jnp.exp(btotal) * came + before, before)
            nbtotal_ref[d, pl.ds(h, 1), :] = jnp.where(takes, btotal + came_total, btotal)
            state = jnp.where(
                takes, jnp.exp(total) * came + state, jnp.exp(came_total) * state + came
            )
            total = total + came_total
            nstate_ref[d, h] = state
            ntotal_ref[d, pl.ds(h, 1), :] = total
            states.append(state)
            if after is None:
                pack(send_ref, d, h, state, total)
        if after is not None:
            send_ref[h] = jnp.where((me & after) != 0, states[1], states[0]).astype(bf16)


def local_kernel(heads, q_ref, v_ref, f_ref, r_ref, fg_ref, rg_ref, ex_ref,
                 inner_ref, df_ref, db_ref, state_ref, total_ref, send_ref):
    rows = q_ref.shape[0]
    width = q_ref.shape[1] // heads
    t = lax.broadcasted_iota(jnp.int32, (rows, rows), 0)
    s = lax.broadcasted_iota(jnp.int32, (rows, rows), 1)
    lower, upper = s <= t, s >= t
    for h in range(heads):
        cols = pl.ds(h * width, width)
        ql = q_ref[:, cols].astype(f32)
        q = ql / (1.0 + jnp.exp(-ql))
        v = v_ref[:, cols]
        extra = ex_ref[:, pl.ds(h, 1)]
        scores = jnp.zeros((rows, rows), f32)
        for d, (raw_ref, gap_ref, tri, d_ref) in enumerate(
            ((f_ref, fg_ref, lower, df_ref), (r_ref, rg_ref, upper, db_ref))
        ):
            raw = raw_ref[:, cols].astype(f32)
            key = gap_ref[:, cols] * (1.0 / (1.0 + jnp.exp(raw)))
            log = jnp.log1p(-key) + extra
            run = jnp.dot(tri.astype(f32), log, precision=highest, preferred_element_type=f32)
            last = run[rows - 1 :, :] if d == 0 else run[:1, :]
            dq = (q * jnp.exp(run)).astype(bf16)
            ki = (key * jnp.exp(-run)).astype(bf16)
            ks = (key * jnp.exp(last - run)).astype(bf16)
            part = lax.dot_general(dq, ki, (((1,), (1,)), ((), ())), preferred_element_type=f32)
            scores = scores + jnp.where(tri, part, 0.0)
            d_ref[:, cols] = dq
            state = lax.dot_general(v, ks, (((0,), (0,)), ((), ())), preferred_element_type=f32)
            state_ref[d, h] = state
            total_ref[d, pl.ds(h, 1), :] = last
            pack(send_ref, d, h, state, last)
        inner_ref[:, cols] = jnp.dot(scores.astype(bf16), v, preferred_element_type=f32)


def mix_kernel(bit, heads, inner_ref, df_ref, db_ref, came_ref, before_ref, btotal_ref,
               gate_ref, gain_ref, out_ref):
    width = inner_ref.shape[1] // heads
    high = (lax.axis_index("sp") & bit) != 0
    for h in range(heads):
        cols = pl.ds(h * width, width)
        mixed = inner_ref[:, cols]
        came = came_ref[h].astype(f32)
        for d, d_ref in enumerate((df_ref, db_ref)):
            takes = high if d == 0 else jnp.logical_not(high)
            before = before_ref[d, h]
            state = jnp.where(
                takes, jnp.exp(btotal_ref[d, pl.ds(h, 1), :]) * came + before, before
            )
            mixed = mixed + lax.dot_general(
                d_ref[:, cols], state.astype(bf16), (((1,), (1,)), ((), ())),
                preferred_element_type=f32,
            )
        normed = (
            mixed
            * lax.rsqrt(jnp.mean(mixed * mixed, axis=1, keepdims=True) + head_eps)
            * gain_ref[...]
        )
        gl = gate_ref[:, cols].astype(f32)
        out_ref[:, cols] = (normed * (gl / (1.0 + jnp.exp(-gl)))).astype(bf16)


def ordered(x, far, near, place):
    _, model = x.shape
    slab = model // (far * near)
    blocks = [
        jnp.concatenate(
            [x[:, (z * near + r) * slab : (z * near + r + 1) * slab] for z in range(far)], axis=1
        )
        for r in range(near)
    ]
    return unxor(blocks, place)


def unordered(blocks, far, near, place):
    blocks = unxor(blocks, place)
    slab = blocks[0].shape[1] // far
    return jnp.concatenate(
        [blocks[r][:, z * slab : (z + 1) * slab] for z in range(far) for r in range(near)], axis=1
    )


def middle_kernel(cores, far, near, *refs):
    gated, output, residual, gains, biases = (refs[i * cores : (i + 1) * cores] for i in range(5))
    middle_ref, send_ref = refs[5 * cores :]
    core = lax.axis_index("tp")
    width = gated[0].shape[1]
    parts = []
    for b in range(cores):
        mixer = alpha_mix * residual[b][...].astype(f32)
        for m in range(cores):
            at = pl.ds(pl.multiple_of((core ^ m) * width, width), width)
            mixer = mixer + jnp.dot(gated[m][...], output[b][at, :], preferred_element_type=f32)
        parts.append(mixer)
    model = cores * parts[0].shape[1]
    mean = sum(jnp.sum(p, axis=1, keepdims=True) for p in parts) / model
    parts = [p - mean for p in parts]
    var = sum(jnp.sum(p * p, axis=1, keepdims=True) for p in parts) / model
    scale = lax.rsqrt(var + norm_eps)
    parts = [p * scale * gains[b][...] + biases[b][...] for b, p in enumerate(parts)]
    whole = jnp.concatenate(unxor(parts, core), axis=1)
    middle_ref[...] = whole.astype(bf16)
    near_place = lax.rem(lax.axis_index("sp"), near)
    blocks = ordered(whole.astype(bf16).astype(f32), far, near, near_place)
    share = near // cores
    halves = [
        jnp.concatenate(blocks[c * share : (c + 1) * share], axis=1) for c in range(cores)
    ]
    send_ref[...] = unxor(halves, core)[0].astype(bf16)


def deal_kernel(far, near, gate_ref, up_ref, *outs):
    place = lax.axis_index("sp") // near
    units = gate_ref.shape[1] // far
    for i, ref in enumerate((gate_ref, up_ref)):
        whole = ref[...].astype(f32).T
        pieces = [whole[z * units : (z + 1) * units] for z in range(far)]
        for out, piece in zip(outs, unxor(pieces, place)):
            out[i] = piece.astype(bf16)


def stack_kernel(far, near, *refs):
    place = lax.axis_index("sp") // near
    for i in range(2):
        pieces = unxor([r[i].astype(f32) for r in refs[:far]], place)
        refs[far + i][...] = jnp.concatenate(pieces, axis=1).astype(bf16)


def across(x, w):
    return lax.dot_general(x, w, (((1,), (1,)), ((), ())), preferred_element_type=f32)


def hidden_kernel(cores, near, *refs):
    rows = refs[:cores]
    gates, ups = (refs[cores + i * near : cores + (i + 1) * near] for i in range(2))
    out_ref = refs[-1]
    core = lax.axis_index("tp")
    share = near // cores
    deep = gates[0].shape[1]
    lanes = unxor([r[...] for r in rows], core)
    gate = up = 0.0
    for j in range(near):
        x = lanes[j // share][:, (j % share) * deep : (j % share + 1) * deep]
        gate = gate + across(x, gates[j][...])
        up = up + across(x, ups[j][...])
    out_ref[...] = (gate / (1.0 + jnp.exp(-gate)) * up).astype(bf16)


def down_kernel(cores, near, hidden_ref, *refs):
    first, second, outs = refs[:near], refs[near : 2 * near], refs[2 * near :]
    core = lax.axis_index("tp")
    share = near // cores
    half = first[0].shape[0]
    a, b = hidden_ref[:, :half], hidden_ref[:, half:]
    halves = []
    for c in range(cores):
        halves.append(
            jnp.concatenate(
                [
                    jnp.dot(a, first[j][...], preferred_element_type=f32)
                    + jnp.dot(b, second[j][...], preferred_element_type=f32)
                    for j in range(c * share, (c + 1) * share)
                ],
                axis=1,
            ).astype(bf16)
        )
    for out, y in zip(outs, unxor(halves, core)):
        out[...] = y


def final_kernel(cores, far, near, *refs):
    feeds = refs[:cores]
    middle_ref, gain_ref, bias_ref, out_ref = refs[cores:]
    core = lax.axis_index("tp")
    near_place = lax.rem(lax.axis_index("sp"), near)
    whole = unxor([f[...].astype(f32) for f in feeds], core)
    share = near // cores
    deep = whole[0].shape[1] // share
    blocks = [
        whole[j // share][:, (j % share) * deep : (j % share + 1) * deep] for j in range(near)
    ]
    x = alpha_mix * middle_ref[...].astype(f32) + unordered(blocks, far, near, near_place)
    mean = jnp.mean(x, axis=1, keepdims=True)
    x = x - mean
    x = x * lax.rsqrt(jnp.mean(x * x, axis=1, keepdims=True) + norm_eps)
    width = out_ref.shape[1]
    mine = unxor([x[:, c * width : (c + 1) * width] for c in range(cores)], core)[0]
    out_ref[...] = (mine * gain_ref[...] + bias_ref[...]).astype(bf16)


def call(body, outs, *args, flops=0):
    size = sum(math.prod(a.shape) * a.dtype.itemsize for a in list(outs) + list(args))
    return pl.pallas_call(
        body,
        out_shape=tuple(outs),
        cost_estimate=pl.CostEstimate(flops=flops, bytes_accessed=size * 4, transcendentals=0),
        compiler_params=pltpu.CompilerParams(vmem_limit_bytes=56 * 1024 * 1024),
    )(*args)


def spread(own, near, order):
    blocks = {0: own}
    for bit in order:
        for m, b in list(blocks.items()):
            blocks[m ^ bit] = swap(b, "sp", bit)
    return [blocks[j] for j in range(near)]


def shards(
    query_logits, value_rows, onward_forget_logits, reverse_forget_logits, output_gate_logits,
    onward_floor_gap, reverse_floor_gap, extra_log_decay, per_head_gain, residual, output_matrix,
    inner_norm_gain, inner_norm_bias, gate_matrix, up_matrix, down_matrix,
    closing_norm_gain, closing_norm_bias,
):
    count, cores = lax.axis_size("sp"), lax.axis_size("tp")
    me = lax.axis_index("sp")
    far = math.gcd(count, 4)
    near = count // far
    rows, width = query_logits.shape
    heads = extra_log_decay.shape[1]
    chan = width // heads
    share = residual.shape[1]
    model = share * cores
    units = gate_matrix.shape[1] // far
    place = me // near
    like = jax.ShapeDtypeStruct
    states = (like((2, heads, chan, chan), f32), like((2, heads, chan), f32))
    packed = like((2, heads, chan + 16, chan), bf16)

    inner, df, db, state, total, sent = call(
        functools.partial(local_kernel, heads),
        (like((rows, width), f32), like((rows, width), bf16), like((rows, width), bf16))
        + states + (packed,),
        query_logits, value_rows, onward_forget_logits, reverse_forget_logits,
        onward_floor_gap[None], reverse_floor_gap[None], extra_log_decay,
    )

    def dealt(cuts):
        blocks = [swap(c, "sp", s * near) if s else c for s, c in enumerate(cuts)]
        return unxor(blocks, place)

    units_like = like((2, units, gate_matrix.shape[0]), bf16)
    cuts = call(
        functools.partial(deal_kernel, far, near), [units_like] * far, gate_matrix, up_matrix
    )
    gate_own, up_own = call(
        functools.partial(stack_kernel, far, near),
        [like((units, far * gate_matrix.shape[0]), bf16)] * 2,
        *[swap(c, "sp", s * near) if s else c for s, c in enumerate(cuts)],
    )
    down_matrix, _ = lax.optimization_barrier((down_matrix, gate_own[:8, :128]))
    down = dealt(
        [lax.dynamic_slice_in_dim(down_matrix, (place ^ s) * units, units, 0) for s in range(far)]
    )
    half = (units // 2 + 127) // 128 * 128
    bits = bits_of(near)
    gates = spread(gate_own, near, bits)
    ups = spread(up_own, near, bits[::-1])
    first = spread(jnp.concatenate([d[:half] for d in down], axis=1), near, bits)
    second = spread(jnp.concatenate([d[half:] for d in down], axis=1), near, bits[::-1])

    residuals = tp_blocks(residual)
    vectors = tp_blocks(jnp.stack([inner_norm_gain, inner_norm_bias]))
    outputs = tp_blocks(output_matrix)

    steps = bits_of(count)
    before, before_total = state, total
    for i, bit in enumerate(steps[:-1]):
        last = i == len(steps) - 2
        came = swap(sent, "sp", bit)
        state, total, before, before_total, sent = call(
            functools.partial(join_kernel, bit, steps[-1] if last else None, i == 0),
            states + states + (like((heads, chan, chan), bf16) if last else packed,),
            came, state, total, before, before_total,
        )
    came = swap(sent, "sp", steps[-1])
    (gated,) = call(
        functools.partial(mix_kernel, steps[-1], heads),
        (like((rows, width), bf16),),
        inner, df, db, came, before, before_total, output_gate_logits, per_head_gain[None],
    )
    gated = tp_blocks(gated)
    middle, ready = call(
        functools.partial(middle_kernel, cores, far, near),
        (like((rows, model), bf16), like((rows, share), bf16)),
        *gated, *outputs, *residuals, *[v[:1] for v in vectors], *[v[1:] for v in vectors],
        flops=2 * rows * width * cores * model,
    )

    lines = jnp.concatenate(
        [ready] + [swap(ready, "sp", s * near) for s in range(1, far)], axis=0
    )
    lines = tp_blocks(lines)
    (hidden,) = call(
        functools.partial(hidden_kernel, cores, near),
        (like((far * rows, units), bf16),),
        *lines, *gates, *ups,
        flops=4 * far * rows * model * units,
    )
    sums = call(
        functools.partial(down_kernel, cores, near),
        [like((far * rows, share), bf16)] * cores,
        hidden, *first, *second,
        flops=2 * far * rows * model * units,
    )
    feed = sums[0].astype(f32)
    for m in range(1, cores):
        feed = feed + swap(sums[m], "tp", m).astype(f32)
    feed = feed.astype(bf16)
    mine = feed[:rows].astype(f32)
    for s in range(1, far):
        mine = mine + swap(feed[s * rows : (s + 1) * rows], "sp", s * near).astype(f32)
    (out,) = call(
        functools.partial(final_kernel, cores, far, near),
        (like((rows, share), bf16),),
        *tp_blocks(mine.astype(bf16)), middle, closing_norm_gain[None], closing_norm_bias[None],
    )
    return out


def solution(mesh):
    a, b = P("sp", "tp"), P("tp")
    placed = (a, a, a, a, a, b, b, a, P(), a, P(None, "tp"), b, b, a, a, P("tp", "sp"), b, b)

    return jax.shard_map(
        shards, mesh=mesh, in_specs=placed, out_specs=P("sp", "tp"), check_vma=False
    )
```
